32 devices in a mesh: sp: 8 (over z, y), tp: 4 (over x, core).
Axes of the slice: x: 2, y: 2, z: 4, core: 2. Of those that a mesh axis runs over, the one named last changes fastest.
Arguments:
- stream: bfloat16 [8192, 4096], P('sp', 'tp'), may hold values from -11 to 11
- norm_gain: bfloat16 [3, 4096], P(None, 'tp'), may hold values from 0.099609375 to 1.8984375
- pool_weight: bfloat16 [3, 4, 1024, 1024], P(None, 'tp', 'sp'), may hold values from -0.1875 to 0.1875
- pool_scale: bfloat16 [3, 4096], P(None, 'tp'), may hold values from 0.099609375 to 1.8984375
Outputs:
- mixed: bfloat16 [8192, 4096], P('sp', 'tp')
The draws below stay inside these ranges and needn't reach their ends.
All inputs are finite; a program needn't handle non-finite values.
Results may differ from the reference program's by a relative error of at most 0.015.
Values may be sent and summed in bfloat16 or wider, within the bound.
A program may use at most 64 MiB of HBM per device.

```python
import jax
import jax.numpy as jnp
from jax import lax

D = 4096
POOL_GROUPS = 4
LAYERS = 3
GC = 1024
TOKENS = 8192


def draw_stream(key, part):
    noise_key, perm_key, row_key = jax.random.split(key, 3)
    levels = 0.5 * 3.0 ** (jnp.arange(POOL_GROUPS, dtype=jnp.float32) / (POOL_GROUPS - 1))
    levels = jax.random.permutation(perm_key, levels)
    column_scale = jnp.repeat(levels, GC)
    base_vals = jax.random.truncated_normal(noise_key, -6.0, 6.0, (TOKENS, D), jnp.float32)
    return (base_vals * column_scale[None, :]).astype(jnp.bfloat16)


def shard_levels(key, extent, cuts, low, largest):
    gain = 1.0
    for dim, shards_of in cuts:
        draws = jax.random.uniform(jax.random.fold_in(jax.random.fold_in(key, 6), dim), (shards_of,), jnp.float32, low / len(cuts), largest / len(cuts))
        gain = gain * jnp.repeat(jnp.exp(draws), extent[dim] // shards_of).reshape((-1,) + (1,) * (len(extent) - 1 - dim))
    return gain


def noise(key, shape, scale, bound, cuts=(), kind=jnp.bfloat16):
    factor_of = shard_levels(key, shape, cuts, -0.22, 0.18) if cuts else 1.0
    drawn = jax.random.normal(key, shape, jnp.float32) * scale * factor_of
    return jnp.minimum(jnp.maximum(drawn, -bound), bound).astype(kind)


def setup_inputs(seed: int = 0) -> dict:
    splits = jax.random.split(jax.random.key(seed), 5)
    stream = draw_stream(jax.random.fold_in(splits[4], 71), 0)
    norm_gain = jnp.clip(1.0 + 0.18 * jax.random.normal(splits[1], (LAYERS, D), jnp.float32), 0.099609375, 1.8984375).astype(jnp.bfloat16)
    pool_weight = noise(splits[2], (LAYERS, POOL_GROUPS, GC, GC), GC ** -0.5, 0.1875, ((1, 4), (2, 8)))
    pool_scale = jnp.clip(1.0 + 0.18 * jax.random.normal(splits[3], (LAYERS, D), jnp.float32), 0.099609375, 1.8984375).astype(jnp.bfloat16)
    return {"stream": stream, "norm_gain": norm_gain, "pool_weight": pool_weight, "pool_scale": pool_scale}


norm_eps = 1e-06

def centred_mean(values, half_width):
    length = values.shape[0]
    sums = jnp.concatenate([jnp.zeros((1, values.shape[1]), jnp.float32), jnp.cumsum(values, axis=0)], axis=0)
    positions = jnp.arange(length)
    low_end = jnp.maximum(positions - half_width, 0)
    high_end = jnp.minimum(positions + half_width, length)
    return (sums[high_end] - sums[low_end]) / (high_end - low_end).astype(jnp.float32)[:, None]

def reference(stream, norm_gain, pool_weight, pool_scale):
    current = stream
    for layer_idx in range(LAYERS):
        stream_f = current.astype(jnp.float32)
        meansq = lax.optimization_barrier(jnp.mean(stream_f * stream_f, axis=1, keepdims=True))
        normed = (stream_f * lax.rsqrt(meansq + norm_eps) * norm_gain[layer_idx].astype(jnp.float32)).astype(jnp.bfloat16)
        pieces = []
        for group in range(POOL_GROUPS):
            members = normed[:, group * GC:(group + 1) * GC].astype(jnp.float32)
            pooled = (centred_mean(members, 2 ** group) - members).astype(jnp.bfloat16)
            pieces.append(jnp.dot(pooled, pool_weight[layer_idx, group], preferred_element_type=jnp.float32))
        branch = jnp.concatenate(pieces, axis=1)
        current = (stream_f + branch * pool_scale[layer_idx].astype(jnp.float32)).astype(jnp.bfloat16)
    return current
```

```python
import functools

import jax
import jax.numpy as jnp
from jax import lax
from jax.experimental import pallas as pl
from jax.experimental.pallas import tpu as pltpu
from jax.sharding import PartitionSpec as P

D = 4096
POOL_GROUPS = 4
NORM_EPS = 1e-06
PAD = 64
HALO = 32
TILE = 128
DOWN, UP, ACROSS = 0, 1, 2
MESH = pl.DeviceIdType.MESH


def unit_list(layers, width):
    eighth = width // 8
    units = []
    for layer in range(layers):
        along = 2 * eighth if layer == 0 else eighth
        cuts = [4 * eighth, width - along]
        if layer == layers - 1:
            cuts = [4 * eighth, 6 * eighth, width - along]
        units.append((layer, width - along, along, True))
        first = 0
        for cut in cuts:
            units.append((layer, first, cut - first, False))
            first = cut
    return units


def kernel(cfg, x_hbm, w_hbm, gain_ref, scale_ref, o_hbm, xs, ns, ps, ws, ss_own, ss_in,
           load_sem, halo_send, halo_recv, ss_send, ss_recv, w_send, w_recv, out_sem):
    layers, rows, width, shard_rows, n_sp, n_tp, in_kernel = cfg
    sp, tp = lax.axis_index("sp"), lax.axis_index("tp")
    line = n_sp // 2
    z, y = sp // 2, sp % 2
    units = unit_list(layers, width)
    total_rows = rows + 2 * PAD
    tiles = total_rows // TILE
    seq_total = rows * n_sp
    base_pos = sp * rows - PAD
    half = jnp.left_shift(jnp.int32(1), tp)

    has_down, has_up = z > 0, z < line - 1
    has_prev, has_next = sp > 0, sp < n_sp - 1
    target = {DOWN: (sp - 2, tp), UP: (sp + 2, tp), ACROSS: (z * 2 + (1 - y), tp)}

    x_load = pltpu.make_async_copy(x_hbm, xs.at[pl.ds(PAD, rows)], load_sem.at[layers])
    own_rows = pl.ds(pl.multiple_of(sp * shard_rows, shard_rows), shard_rows)
    if in_kernel:
        w_loads = [
            pltpu.make_async_copy(w_hbm.at[l, 0], ws.at[l, own_rows], load_sem.at[l])
            for l in range(layers)
        ]
    else:
        w_loads = [
            pltpu.make_async_copy(w_hbm.at[l, 0], ws.at[l], load_sem.at[l])
            for l in range(layers)
        ]
    w_loads[0].start()
    x_load.start()
    for l in range(1, layers):
        w_loads[l].start()

    barrier = pltpu.get_barrier_semaphore()

    def greet(device):
        pl.semaphore_signal(barrier, inc=1, device_id=device, device_id_type=MESH)

    expected = jnp.int32(n_tp - 1)
    for p in range(1, n_tp):
        greet((sp, lax.rem(tp + p, n_tp)))
    pl.when(has_prev)(lambda: greet((sp - 1, tp)))
    pl.when(has_next)(lambda: greet((sp + 1, tp)))
    expected = expected + has_prev.astype(jnp.int32) + has_next.astype(jnp.int32)
    if in_kernel:
        greet(target[ACROSS])
        pl.when(has_down)(lambda: greet(target[DOWN]))
        pl.when(has_up)(lambda: greet(target[UP]))
        expected = expected + 1 + has_down.astype(jnp.int32) + has_up.astype(jnp.int32)

    zero = jnp.zeros((PAD, width), jnp.bfloat16)
    ns[pl.ds(0, PAD)] = zero
    ns[pl.ds(total_rows + PAD, PAD)] = zero
    xs[pl.ds(0, PAD - HALO)] = zero[: PAD - HALO]
    xs[pl.ds(PAD + rows + HALO, PAD - HALO)] = zero[: PAD - HALO]

    @pl.when(jnp.logical_not(has_prev))
    def _():
        xs[pl.ds(PAD - HALO, HALO)] = zero[:HALO]

    @pl.when(jnp.logical_not(has_next))
    def _():
        xs[pl.ds(PAD + rows, HALO)] = zero[:HALO]

    pl.semaphore_wait(barrier, expected)

    to_next = pltpu.make_async_remote_copy(
        x_hbm.at[pl.ds(rows - HALO, HALO)], xs.at[pl.ds(PAD - HALO, HALO)],
        halo_send.at[0], halo_recv.at[0], device_id=(sp + 1, tp), device_id_type=MESH)
    to_prev = pltpu.make_async_remote_copy(
        x_hbm.at[pl.ds(0, HALO)], xs.at[pl.ds(PAD + rows, HALO)],
        halo_send.at[1], halo_recv.at[1], device_id=(sp - 1, tp), device_id_type=MESH)
    pl.when(has_next)(lambda: to_next.start())
    pl.when(has_prev)(lambda: to_prev.start())

    def piece(u, j, col):
        layer, first, columns, _ = units[u]
        start = pl.multiple_of((j * 2 + col) * shard_rows, shard_rows)
        return ws.at[layer, pl.ds(start, shard_rows), pl.ds(first, columns)]

    def copy(way, u, j, col):
        at = j * 2 + col
        return pltpu.make_async_remote_copy(
            piece(u, j, col), piece(u, j, col), w_send.at[way, u, at], w_recv.at[u, at],
            device_id=target[way], device_id_type=MESH)

    def arrive(u, j, col):
        copy(ACROSS, u, j, col).wait_recv()

    def send_own(u):
        pl.when(has_down)(lambda: copy(DOWN, u, z, y).start())
        pl.when(has_up)(lambda: copy(UP, u, z, y).start())
        copy(ACROSS, u, z, y).start()

    def pass_own_row(u):
        arrive(u, z, 1 - y)
        pl.when(has_down)(lambda: copy(DOWN, u, z, 1 - y).start())
        pl.when(has_up)(lambda: copy(UP, u, z, 1 - y).start())

    def forward(u, step):
        along = units[u][3]

        def hop(j, way, more):
            arrive(u, j, y)
            pl.when(more)(lambda: copy(way, u, j, y).start())
            if along:
                arrive(u, j, 1 - y)
                pl.when(more)(lambda: copy(way, u, j, 1 - y).start())
            else:
                copy(ACROSS, u, j, y).start()

        pl.when(z + step < line)(lambda: hop(z + step, DOWN, has_down))
        pl.when(z - step >= 0)(lambda: hop(z - step, UP, has_up))

    def arrive_across(u):
        if not units[u][3]:
            for j in range(line):
                arrive(u, j, 1 - y)

    def tile_rows(i):
        return pl.ds(pl.multiple_of(i * TILE, TILE), TILE)

    def square_sums(layer):
        @pl.loop(0, tiles)
        def _(i):
            part = jnp.zeros((TILE, 128), jnp.float32)
            for c in range(width // 128):
                v = xs[tile_rows(i), pl.ds(c * 128, 128)].astype(jnp.float32)
                part = part + v * v
            ss_own[layer, pl.ds(i, 1)] = jnp.sum(part.T, axis=0, keepdims=True)

    def ss_copy(layer, p):
        return pltpu.make_async_remote_copy(
            ss_own.at[layer], ss_in.at[layer, p - 1], ss_send.at[layer, p - 1], ss_recv.at[layer, p - 1],
            device_id=(sp, lax.rem(tp + p, n_tp)), device_id_type=MESH)

    def send_sums(layer):
        square_sums(layer)
        for p in range(1, n_tp):
            ss_copy(layer, p).start()

    def wait_sums(layer):
        for p in range(1, n_tp):
            ss_copy(layer, p).wait()

    def normalise(layer, lo, hi):
        @pl.loop(lo, hi)
        def _(i):
            total = ss_own[layer, pl.ds(i, 1)]
            for p in range(1, n_tp):
                total = total + ss_in[layer, p - 1, pl.ds(i, 1)]
            factor = lax.rsqrt(total / D + NORM_EPS)
            pos = base_pos + i * TILE + lax.broadcasted_iota(jnp.int32, (1, TILE), 1)
            factor = jnp.where((pos >= 0) & (pos < seq_total), factor, 0.0)
            column = jnp.broadcast_to(factor, (TILE, TILE)).T
            for c in range(width // 128):
                cols = pl.ds(c * 128, 128)
                v = xs[tile_rows(i), cols].astype(jnp.float32)
                g = gain_ref[layer : layer + 1, cols].astype(jnp.float32)
                ns[pl.ds(pl.multiple_of(PAD + i * TILE, 64), TILE), cols] = (v * column * g).astype(jnp.bfloat16)

    window = TILE + 2 * PAD

    def pool(lo, hi):
        @pl.loop(lo, hi)
        def _(i):
            offset = (
                lax.broadcasted_iota(jnp.int32, (TILE, window), 1)
                - lax.broadcasted_iota(jnp.int32, (TILE, window), 0)
                - PAD
            )
            pos = base_pos + i * TILE + lax.broadcasted_iota(jnp.int32, (TILE, window), 0)
            count = jnp.minimum(pos + half, seq_total) - jnp.maximum(pos - half, 0)
            count = jnp.maximum(count, 1).astype(jnp.float32)
            band = jnp.where((offset >= -half) & (offset < half), 1.0, 0.0)
            band = (band - jnp.where(offset == 0, count, 0.0)).astype(jnp.bfloat16)
            inverse = 1.0 / count[:, :1]
            rows_in = pl.ds(pl.multiple_of(i * TILE, TILE), window)
            for c in range(width // 256):
                cols = pl.ds(c * 256, 256)
                sums = jnp.dot(band, ns[rows_in, cols], preferred_element_type=jnp.float32)
                ps[tile_rows(i), cols] = (sums * inverse).astype(jnp.bfloat16)

    def mix(layer, first_row, block, first, columns):
        cols = pl.ds(first, columns)
        at = pl.ds(pl.multiple_of(first_row, 64), block)
        branch = jnp.dot(ps[at], ws[layer, :, cols], preferred_element_type=jnp.float32)
        s = scale_ref[layer : layer + 1, cols].astype(jnp.float32)
        xs[at, cols] = (xs[at, cols].astype(jnp.float32) + branch * s).astype(jnp.bfloat16)

    third = tiles // 3
    thirds = [(0, third), (third, 2 * third), (2 * third, tiles)]

    def mix_block(layer, lo, hi):
        def run():
            for c in range(width // 256):
                mix(layer, lo * TILE, (hi - lo) * TILE, c * 256, 256)
        return run

    def prepare(layer):
        work = [lambda: send_sums(layer), lambda: None]
        first = [True]

        def norm(lo, hi):
            if first[0]:
                wait_sums(layer)
                first[0] = False
            normalise(layer, lo, hi)

        work += [functools.partial(norm, lo, hi) for lo, hi in thirds]
        work += [functools.partial(pool, lo, hi) for lo, hi in thirds]
        return work

    def start_work():
        x_load.wait()
        pl.when(has_prev)(lambda: to_next.wait_recv())
        pl.when(has_next)(lambda: to_prev.wait_recv())

    if in_kernel:
        count = len(units)
        w_loads[0].wait()
        waited = 0
        for u in range(2):
            send_own(u)
        ahead = 2
        tasks = [start_work] + prepare(0)
        for u in range(count):
            layer, along = units[u][0], units[u][3]
            if ahead < count:
                if units[ahead][0] > waited:
                    waited = units[ahead][0]
                    w_loads[waited].wait()
                send_own(ahead)
                ahead += 1
            if along:
                pass_own_row(u)
            for step in range(1, line):
                forward(u, step)
                if tasks:
                    tasks.pop(0)()
            if along and layer > 0:
                while tasks:
                    tasks.pop(0)()
                for v in range(count):
                    if units[v][0] == layer - 1:
                        arrive_across(v)
                tasks = [mix_block(layer - 1, lo, hi) for lo, hi in thirds] + prepare(layer)
        while tasks:
            tasks.pop(0)()
    else:
        start_work()
        for layer in range(layers):
            for task in prepare(layer):
                task()
            w_loads[layer].wait()
            if layer < layers - 1:
                for lo, hi in thirds:
                    mix_block(layer, lo, hi)()

    outs = []
    for u, (layer, first, columns, _) in enumerate(units):
        if layer < layers - 1:
            continue
        if in_kernel:
            arrive_across(u)

        @pl.loop(0, rows // 256)
        def _(i):
            mix(layer, PAD + i * 256, 256, first, columns)

        out = pltpu.make_async_copy(
            xs.at[pl.ds(PAD, rows), pl.ds(first, columns)], o_hbm.at[:, pl.ds(first, columns)], out_sem.at[len(outs)])
        out.start()
        outs.append(out)

    pl.when(has_next)(lambda: to_next.wait_send())
    pl.when(has_prev)(lambda: to_prev.wait_send())
    if in_kernel:
        for u in range(len(units)):
            along = units[u][3]
            for j in range(line):
                def done(way, col):
                    copy(way, u, j, col).wait_send()

                @pl.when(has_down & (j >= z))
                def _():
                    done(DOWN, y)
                    if along:
                        done(DOWN, 1 - y)

                @pl.when(has_up & (j <= z))
                def _():
                    done(UP, y)
                    if along:
                        done(UP, 1 - y)

                if along:
                    pl.when(z == j)(lambda: done(ACROSS, y))
                else:
                    done(ACROSS, y)
    for out in outs:
        out.wait()


def solution(mesh):
    n_sp, n_tp = mesh.shape["sp"], mesh.shape["tp"]
    in_kernel = n_sp % 2 == 0 and n_sp <= 16

    def local(stream, norm_gain, pool_weight, pool_scale):
        rows, _ = stream.shape
        layers, per_dev, shard_rows, width = pool_weight.shape
        assert per_dev == 1 and n_tp == POOL_GROUPS
        if not in_kernel:
            pool_weight = lax.all_gather(pool_weight, "sp", axis=2, tiled=True)
        total_rows = rows + 2 * PAD
        units = len(unit_list(layers, width)) if in_kernel else 1
        dma = pltpu.SemaphoreType.DMA
        any_space = pl.BlockSpec(memory_space=pl.ANY)
        vmem = pl.BlockSpec(memory_space=pltpu.VMEM)
        return pl.pallas_call(
            functools.partial(kernel, (layers, rows, width, shard_rows, n_sp, n_tp, in_kernel)),
            out_shape=jax.ShapeDtypeStruct((rows, width), jnp.bfloat16),
            in_specs=[any_space, any_space, vmem, vmem],
            out_specs=any_space,
            scratch_shapes=[
                pltpu.VMEM((total_rows, width), jnp.bfloat16),
                pltpu.VMEM((total_rows + 2 * PAD, width), jnp.bfloat16),
                pltpu.VMEM((total_rows, width), jnp.bfloat16),
                pltpu.VMEM((layers, width, width), jnp.bfloat16),
                pltpu.VMEM((layers, 16, TILE), jnp.float32),
                pltpu.VMEM((layers, n_tp - 1, 16, TILE), jnp.float32),
                dma((layers + 1,)),
                dma((2,)),
                dma((2,)),
                dma((layers, n_tp - 1)),
                dma((layers, n_tp - 1)),
                dma((3, units, n_sp)),
                dma((units, n_sp)),
                dma((4,)),
            ],
            compiler_params=pltpu.CompilerParams(
                collective_id=0, has_side_effects=True, vmem_limit_bytes=60 * 2**20
            ),
        )(stream, pool_weight, norm_gain, pool_scale)

    placed = (P("sp", "tp"), P(None, "tp"), P(None, "tp", "sp", None), P(None, "tp"))
    return jax.shard_map(
        local, mesh=mesh, in_specs=placed, out_specs=P("sp", "tp"), check_vma=False
    )
```

```python
import functools

import jax
import jax.numpy as jnp
from jax import lax
from jax.experimental import pallas as pl
from jax.experimental.pallas import tpu as pltpu
from jax.sharding import PartitionSpec as P

D = 4096
POOL_GROUPS = 4
NORM_EPS = 1e-06
PAD = 64
HALO = 32
TILE = 128
DOWN, UP, ACROSS = 0, 1, 2
MESH = pl.DeviceIdType.MESH


LEAD, SKEW, EARLY = 5, 3, 2
MIX_AT = 6


def unit_list(layers, width):
    eighth = width // 8
    units = []
    for layer in range(layers):
        sizes = [3, 2, 2] if layer == layers - 1 else [2, 2, 3]
        units.append((layer, 7 * eighth, eighth, True))
        first = 0
        for size in sizes:
            units.append((layer, first * eighth, size * eighth, False))
            first += size
    return units


def kernel(cfg, x_hbm, w_hbm, gain_ref, scale_ref, out_ref, xs, ns, ps, ws, ss_own, ss_in,
           load_sem, halo_send, halo_recv, ss_send, ss_recv, w_send, w_recv):
    layers, rows, width, shard_rows, n_sp, n_tp, in_kernel = cfg
    sp, tp = lax.axis_index("sp"), lax.axis_index("tp")
    line = n_sp // 2
    z, y = sp // 2, sp % 2
    units = unit_list(layers, width)
    total_rows = rows + 2 * PAD
    tiles = total_rows // TILE
    seq_total = rows * n_sp
    base_pos = sp * rows - PAD
    half = jnp.left_shift(jnp.int32(1), tp)

    has_down, has_up = z > 0, z < line - 1
    has_prev, has_next = sp > 0, sp < n_sp - 1
    target = {DOWN: (sp - 2, tp), UP: (sp + 2, tp), ACROSS: (z * 2 + (1 - y), tp)}

    x_load = pltpu.make_async_copy(x_hbm, xs.at[pl.ds(PAD, rows)], load_sem.at[layers])
    own_rows = pl.ds(pl.multiple_of(sp * shard_rows, shard_rows), shard_rows)
    if in_kernel:
        w_loads = [
            pltpu.make_async_copy(w_hbm.at[l, 0], ws.at[l, own_rows], load_sem.at[l])
            for l in range(layers)
        ]
    else:
        w_loads = [
            pltpu.make_async_copy(w_hbm.at[l, 0], ws.at[l], load_sem.at[l])
            for l in range(layers)
        ]
    w_loads[0].start()
    x_load.start()
    for l in range(1, layers):
        w_loads[l].start()

    barrier = pltpu.get_barrier_semaphore()

    def greet(device):
        pl.semaphore_signal(barrier, inc=1, device_id=device, device_id_type=MESH)

    expected = jnp.int32(n_tp - 1)
    for p in range(1, n_tp):
        greet((sp, lax.rem(tp + p, n_tp)))
    pl.when(has_prev)(lambda: greet((sp - 1, tp)))
    pl.when(has_next)(lambda: greet((sp + 1, tp)))
    expected = expected + has_prev.astype(jnp.int32) + has_next.astype(jnp.int32)
    if in_kernel:
        greet(target[ACROSS])
        pl.when(has_down)(lambda: greet(target[DOWN]))
        pl.when(has_up)(lambda: greet(target[UP]))
        expected = expected + 1 + has_down.astype(jnp.int32) + has_up.astype(jnp.int32)

    zero = jnp.zeros((PAD, width), jnp.bfloat16)
    ns[pl.ds(0, PAD)] = zero
    ns[pl.ds(total_rows + PAD, PAD)] = zero
    xs[pl.ds(0, PAD - HALO)] = zero[: PAD - HALO]
    xs[pl.ds(PAD + rows + HALO, PAD - HALO)] = zero[: PAD - HALO]

    @pl.when(jnp.logical_not(has_prev))
    def _():
        xs[pl.ds(PAD - HALO, HALO)] = zero[:HALO]

    @pl.when(jnp.logical_not(has_next))
    def _():
        xs[pl.ds(PAD + rows, HALO)] = zero[:HALO]

    pl.semaphore_wait(barrier, expected)

    to_next = pltpu.make_async_remote_copy(
        x_hbm.at[pl.ds(rows - HALO, HALO)], xs.at[pl.ds(PAD - HALO, HALO)],
        halo_send.at[0], halo_recv.at[0], device_id=(sp + 1, tp), device_id_type=MESH)
    to_prev = pltpu.make_async_remote_copy(
        x_hbm.at[pl.ds(0, HALO)], xs.at[pl.ds(PAD + rows, HALO)],
        halo_send.at[1], halo_recv.at[1], device_id=(sp - 1, tp), device_id_type=MESH)
    pl.when(has_next)(lambda: to_next.start())
    pl.when(has_prev)(lambda: to_prev.start())

    def piece(u, j, col):
        layer, first, columns, _ = units[u]
        start = pl.multiple_of((j * 2 + col) * shard_rows, shard_rows)
        return ws.at[layer, pl.ds(start, shard_rows), pl.ds(first, columns)]

    def copy(way, u, j, col):
        at = j * 2 + col
        return pltpu.make_async_remote_copy(
            piece(u, j, col), piece(u, j, col), w_send.at[way, u, at], w_recv.at[u, at],
            device_id=target[way], device_id_type=MESH)

    def arrive(u, j, col):
        copy(ACROSS, u, j, col).wait_recv()

    def send_own(u):
        pl.when(has_down)(lambda: copy(DOWN, u, z, y).start())
        pl.when(has_up)(lambda: copy(UP, u, z, y).start())
        copy(ACROSS, u, z, y).start()

    def pass_own_row(u):
        arrive(u, z, 1 - y)
        pl.when(has_down)(lambda: copy(DOWN, u, z, 1 - y).start())
        pl.when(has_up)(lambda: copy(UP, u, z, 1 - y).start())

    def forward(u, step):
        along = units[u][3]

        def hop(j, way, more):
            arrive(u, j, y)
            pl.when(more)(lambda: copy(way, u, j, y).start())
            if along:
                arrive(u, j, 1 - y)
                pl.when(more)(lambda: copy(way, u, j, 1 - y).start())
            else:
                copy(ACROSS, u, j, y).start()

        pl.when(z + step < line)(lambda: hop(z + step, DOWN, has_down))
        pl.when(z - step >= 0)(lambda: hop(z - step, UP, has_up))

    def arrive_across(u):
        if not units[u][3]:
            for j in range(line):
                arrive(u, j, 1 - y)

    def tile_rows(i):
        return pl.ds(pl.multiple_of(i * TILE, TILE), TILE)

    def square_sums(layer):
        @pl.loop(0, tiles)
        def _(i):
            part = jnp.zeros((TILE, 128), jnp.float32)
            for c in range(width // 128):
                v = xs[tile_rows(i), pl.ds(c * 128, 128)].astype(jnp.float32)
                part = part + v * v
            ss_own[layer, pl.ds(i, 1)] = jnp.sum(part.T, axis=0, keepdims=True)

    def ss_copy(layer, p):
        return pltpu.make_async_remote_copy(
            ss_own.at[layer], ss_in.at[layer, p - 1], ss_send.at[layer, p - 1], ss_recv.at[layer, p - 1],
            device_id=(sp, lax.rem(tp + p, n_tp)), device_id_type=MESH)

    def send_sums(layer):
        square_sums(layer)
        for p in range(1, n_tp):
            ss_copy(layer, p).start()

    def wait_sums(layer):
        for p in range(1, n_tp):
            ss_copy(layer, p).wait()

    def normalise(layer, lo, hi):
        @pl.loop(lo, hi)
        def _(i):
            total = ss_own[layer, pl.ds(i, 1)]
            for p in range(1, n_tp):
                total = total + ss_in[layer, p - 1, pl.ds(i, 1)]
            factor = lax.rsqrt(total / D + NORM_EPS)
            pos = base_pos + i * TILE + lax.broadcasted_iota(jnp.int32, (1, TILE), 1)
            factor = jnp.where((pos >= 0) & (pos < seq_total), factor, 0.0)
            column = jnp.broadcast_to(factor, (TILE, TILE)).T
            for c in range(width // 128):
                cols = pl.ds(c * 128, 128)
                v = xs[tile_rows(i), cols].astype(jnp.float32)
                g = gain_ref[layer : layer + 1, cols].astype(jnp.float32)
                ns[pl.ds(pl.multiple_of(PAD + i * TILE, 64), TILE), cols] = (v * column * g).astype(jnp.bfloat16)

    window = TILE + 2 * PAD

    def pool(lo, hi):
        @pl.loop(lo, hi)
        def _(i):
            offset = (
                lax.broadcasted_iota(jnp.int32, (TILE, window), 1)
                - lax.broadcasted_iota(jnp.int32, (TILE, window), 0)
                - PAD
            )
            pos = base_pos + i * TILE + lax.broadcasted_iota(jnp.int32, (TILE, window), 0)
            count = jnp.minimum(pos + half, seq_total) - jnp.maximum(pos - half, 0)
            count = jnp.maximum(count, 1).astype(jnp.float32)
            band = jnp.where((offset >= -half) & (offset < half), 1.0, 0.0)
            band = (band - jnp.where(offset == 0, count, 0.0)).astype(jnp.bfloat16)
            inverse = 1.0 / count[:, :1]
            rows_in = pl.ds(pl.multiple_of(i * TILE, TILE), window)
            for c in range(width // 256):
                cols = pl.ds(c * 256, 256)
                sums = jnp.dot(band, ns[rows_in, cols], preferred_element_type=jnp.float32)
                ps[tile_rows(i), cols] = (sums * inverse).astype(jnp.bfloat16)

    def mix(layer, first_row, block, first, columns, out=False):
        cols = pl.ds(first, columns)
        at = pl.ds(pl.multiple_of(first_row, 64), block)
        branch = jnp.dot(ps[at], ws[layer, :, cols], preferred_element_type=jnp.float32)
        s = scale_ref[layer : layer + 1, cols].astype(jnp.float32)
        mixed = (xs[at, cols].astype(jnp.float32) + branch * s).astype(jnp.bfloat16)
        if out:
            out_ref[pl.ds(pl.multiple_of(first_row - PAD, 64), block), cols] = mixed
        else:
            xs[at, cols] = mixed

    third = tiles // 3
    thirds = [(0, third), (third, 2 * third), (2 * third, tiles)]

    def mix_block(layer, lo, hi):
        def run():
            for c in range(width // 256):
                mix(layer, lo * TILE, (hi - lo) * TILE, c * 256, 256)
        return run

    def prepare(layer):
        work = [lambda: send_sums(layer), lambda: None]
        first = [True]

        def norm(lo, hi):
            if first[0]:
                wait_sums(layer)
                first[0] = False
            normalise(layer, lo, hi)

        work += [functools.partial(norm, lo, hi) for lo, hi in thirds]
        work += [functools.partial(pool, lo, hi) for lo, hi in thirds]
        return work

    def start_work():
        x_load.wait()
        pl.when(has_prev)(lambda: to_next.wait_recv())
        pl.when(has_next)(lambda: to_prev.wait_recv())

    if in_kernel:
        w_loads[0].wait()
        loaded = [0]

        def own(u):
            if units[u][0] > loaded[0]:
                loaded[0] = units[u][0]
                w_loads[loaded[0]].wait()
            send_own(u)

        tasks = [start_work] + prepare(0)

        def next_layer(layer):
            while tasks:
                tasks.pop(0)()
            for v in range(len(units)):
                if units[v][0] == layer - 1:
                    arrive_across(v)
            tasks.extend([mix_block(layer - 1, lo, hi) for lo, hi in thirds] + prepare(layer))

        events = []
        place = 0
        for u in range(len(units)):
            events.append((place - LEAD, 0, u, functools.partial(own, u)))
            if units[u][3]:
                events.append((place - EARLY, 1, u, functools.partial(pass_own_row, u)))
            for step in range(1, line):
                events.append((place + SKEW * (step - 1), 2 + step, u, functools.partial(forward, u, step)))
            place += units[u][2] // (width // 8)
        for layer in range(1, layers):
            events.append((8 * layer + MIX_AT, 2, 0, functools.partial(next_layer, layer)))
        for _, kind, _, event in sorted(events, key=lambda e: e[:3]):
            event()
            if kind > 2 and tasks:
                tasks.pop(0)()
        while tasks:
            tasks.pop(0)()
    else:
        start_work()
        for layer in range(layers):
            for task in prepare(layer):
                task()
            w_loads[layer].wait()
            if layer < layers - 1:
                for lo, hi in thirds:
                    mix_block(layer, lo, hi)()

    for u, (layer, first, columns, _) in enumerate(units):
        if layer < layers - 1:
            continue
        if in_kernel:
            arrive_across(u)

        @pl.loop(0, rows // 256)
        def _(i):
            mix(layer, PAD + i * 256, 256, first, columns, out=True)

    pl.when(has_next)(lambda: to_next.wait_send())
    pl.when(has_prev)(lambda: to_prev.wait_send())
    if in_kernel:
        for u in range(len(units)):
            along = units[u][3]
            for j in range(line):
                def done(way, col):
                    copy(way, u, j, col).wait_send()

                @pl.when(has_down & (j >= z))
                def _():
                    done(DOWN, y)
                    if along:
                        done(DOWN, 1 - y)

                @pl.when(has_up & (j <= z))
                def _():
                    done(UP, y)
                    if along:
                        done(UP, 1 - y)

                if along:
                    pl.when(z == j)(lambda: done(ACROSS, y))
                else:
                    done(ACROSS, y)


def solution(mesh):
    n_sp, n_tp = mesh.shape["sp"], mesh.shape["tp"]
    in_kernel = n_sp % 2 == 0 and n_sp <= 16

    def local(stream, norm_gain, pool_weight, pool_scale):
        rows, _ = stream.shape
        layers, per_dev, shard_rows, width = pool_weight.shape
        assert per_dev == 1 and n_tp == POOL_GROUPS
        if not in_kernel:
            pool_weight = lax.all_gather(pool_weight, "sp", axis=2, tiled=True)
        total_rows = rows + 2 * PAD
        units = len(unit_list(layers, width)) if in_kernel else 1
        dma = pltpu.SemaphoreType.DMA
        hbm = pl.BlockSpec(memory_space=pltpu.HBM)
        vmem = pl.BlockSpec(memory_space=pltpu.VMEM)
        return pl.pallas_call(
            functools.partial(kernel, (layers, rows, width, shard_rows, n_sp, n_tp, in_kernel)),
            out_shape=jax.ShapeDtypeStruct((rows, width), jnp.bfloat16),
            in_specs=[hbm, hbm, vmem, vmem],
            out_specs=vmem,
            scratch_shapes=[
                pltpu.VMEM((total_rows, width), jnp.bfloat16),
                pltpu.VMEM((total_rows + 2 * PAD, width), jnp.bfloat16),
                pltpu.VMEM((total_rows, width), jnp.bfloat16),
                pltpu.VMEM((layers, width, width), jnp.bfloat16),
                pltpu.VMEM((layers, 16, TILE), jnp.float32),
                pltpu.VMEM((layers, n_tp - 1, 16, TILE), jnp.float32),
                dma((layers + 1,)),
                dma((2,)),
                dma((2,)),
                dma((layers, n_tp - 1)),
                dma((layers, n_tp - 1)),
                dma((3, units, n_sp)),
                dma((units, n_sp)),
            ],
            compiler_params=pltpu.CompilerParams(
                collective_id=0, has_side_effects=True, vmem_limit_bytes=24 * 2**20
            ),
        )(stream, pool_weight, norm_gain, pool_scale)

    placed = (P("sp", "tp"), P(None, "tp"), P(None, "tp", "sp", None), P(None, "tp"))
    return jax.shard_map(
        local, mesh=mesh, in_specs=placed, out_specs=P("sp", "tp"), check_vma=False
    )
```

```python
import functools

import jax
import jax.numpy as jnp
from jax import lax
from jax.experimental import pallas as pl
from jax.experimental.pallas import tpu as pltpu
from jax.sharding import PartitionSpec as P

D = 4096
POOL_GROUPS = 4
NORM_EPS = 1e-06
PAD = 64
HALO = 32
TILE = 128
DOWN, UP, ACROSS = 0, 1, 2
MESH = pl.DeviceIdType.MESH


LEAD, SKEW, EARLY = 5, 3, 2
MIX_AT = 6


def unit_list(layers, width):
    eighth = width // 8
    units = []
    for layer in range(layers):
        sizes = [3, 2, 2] if layer == layers - 1 else [2, 2, 3]
        units.append((layer, 7 * eighth, eighth, True))
        first = 0
        for size in sizes:
            units.append((layer, first * eighth, size * eighth, False))
            first += size
    return units


def kernel(cfg, x_hbm, w_hbm, gain_hbm, scale_hbm, out_ref, gain_ref, scale_ref, xs, ns, ps, ws, ss_own, ss_in,
           load_sem, halo_send, halo_recv, ss_send, ss_recv, w_send, w_recv, out_sem):
    layers, rows, width, shard_rows, n_sp, n_tp, in_kernel = cfg
    sp, tp = lax.axis_index("sp"), lax.axis_index("tp")
    line = n_sp // 2
    z, y = sp // 2, sp % 2
    units = unit_list(layers, width)
    total_rows = rows + 2 * PAD
    tiles = total_rows // TILE
    seq_total = rows * n_sp
    base_pos = sp * rows - PAD
    half = jnp.left_shift(jnp.int32(1), tp)

    has_down, has_up = z > 0, z < line - 1
    has_prev, has_next = sp > 0, sp < n_sp - 1
    target = {DOWN: (sp - 2, tp), UP: (sp + 2, tp), ACROSS: (z * 2 + (1 - y), tp)}

    x_load = pltpu.make_async_copy(x_hbm, xs.at[pl.ds(PAD, rows)], load_sem.at[layers])
    own_rows = pl.ds(pl.multiple_of(sp * shard_rows, shard_rows), shard_rows)
    if in_kernel:
        w_loads = [
            pltpu.make_async_copy(w_hbm.at[l, 0], ws.at[l, own_rows], load_sem.at[l])
            for l in range(layers)
        ]
    else:
        w_loads = [
            pltpu.make_async_copy(w_hbm.at[l, 0], ws.at[l], load_sem.at[l])
            for l in range(layers)
        ]
    w_loads[0].start()
    x_load.start()
    gain_load = pltpu.make_async_copy(gain_hbm, gain_ref, load_sem.at[layers + 1])
    scale_load = pltpu.make_async_copy(scale_hbm, scale_ref, load_sem.at[layers + 2])
    gain_load.start()
    scale_load.start()
    for l in range(1, layers):
        w_loads[l].start()

    barrier = pltpu.get_barrier_semaphore()

    def greet(device):
        pl.semaphore_signal(barrier, inc=1, device_id=device, device_id_type=MESH)

    expected = jnp.int32(n_tp - 1)
    for p in range(1, n_tp):
        greet((sp, lax.rem(tp + p, n_tp)))
    pl.when(has_prev)(lambda: greet((sp - 1, tp)))
    pl.when(has_next)(lambda: greet((sp + 1, tp)))
    expected = expected + has_prev.astype(jnp.int32) + has_next.astype(jnp.int32)
    if in_kernel:
        greet(target[ACROSS])
        pl.when(has_down)(lambda: greet(target[DOWN]))
        pl.when(has_up)(lambda: greet(target[UP]))
        expected = expected + 1 + has_down.astype(jnp.int32) + has_up.astype(jnp.int32)

    zero = jnp.zeros((PAD, width), jnp.bfloat16)
    ns[pl.ds(0, PAD)] = zero
    ns[pl.ds(total_rows + PAD, PAD)] = zero
    xs[pl.ds(0, PAD - HALO)] = zero[: PAD - HALO]
    xs[pl.ds(PAD + rows + HALO, PAD - HALO)] = zero[: PAD - HALO]

    @pl.when(jnp.logical_not(has_prev))
    def _():
        xs[pl.ds(PAD - HALO, HALO)] = zero[:HALO]

    @pl.when(jnp.logical_not(has_next))
    def _():
        xs[pl.ds(PAD + rows, HALO)] = zero[:HALO]

    pl.semaphore_wait(barrier, expected)

    to_next = pltpu.make_async_remote_copy(
        x_hbm.at[pl.ds(rows - HALO, HALO)], xs.at[pl.ds(PAD - HALO, HALO)],
        halo_send.at[0], halo_recv.at[0], device_id=(sp + 1, tp), device_id_type=MESH)
    to_prev = pltpu.make_async_remote_copy(
        x_hbm.at[pl.ds(0, HALO)], xs.at[pl.ds(PAD + rows, HALO)],
        halo_send.at[1], halo_recv.at[1], device_id=(sp - 1, tp), device_id_type=MESH)
    pl.when(has_next)(lambda: to_next.start())
    pl.when(has_prev)(lambda: to_prev.start())

    def piece(u, j, col):
        layer, first, columns, _ = units[u]
        start = pl.multiple_of((j * 2 + col) * shard_rows, shard_rows)
        return ws.at[layer, pl.ds(start, shard_rows), pl.ds(first, columns)]

    def copy(way, u, j, col):
        at = j * 2 + col
        return pltpu.make_async_remote_copy(
            piece(u, j, col), piece(u, j, col), w_send.at[way, u, at], w_recv.at[u, at],
            device_id=target[way], device_id_type=MESH)

    def arrive(u, j, col):
        copy(ACROSS, u, j, col).wait_recv()

    def send_own(u):
        pl.when(has_down)(lambda: copy(DOWN, u, z, y).start())
        pl.when(has_up)(lambda: copy(UP, u, z, y).start())
        copy(ACROSS, u, z, y).start()

    def pass_own_row(u):
        arrive(u, z, 1 - y)
        pl.when(has_down)(lambda: copy(DOWN, u, z, 1 - y).start())
        pl.when(has_up)(lambda: copy(UP, u, z, 1 - y).start())

    def forward(u, step):
        along = units[u][3]

        def hop(j, way, more):
            arrive(u, j, y)
            pl.when(more)(lambda: copy(way, u, j, y).start())
            if along:
                arrive(u, j, 1 - y)
                pl.when(more)(lambda: copy(way, u, j, 1 - y).start())
            else:
                copy(ACROSS, u, j, y).start()

        pl.when(z + step < line)(lambda: hop(z + step, DOWN, has_down))
        pl.when(z - step >= 0)(lambda: hop(z - step, UP, has_up))

    def arrive_across(u):
        if not units[u][3]:
            for j in range(line):
                arrive(u, j, 1 - y)

    def tile_rows(i):
        return pl.ds(pl.multiple_of(i * TILE, TILE), TILE)

    def square_sums(layer):
        @pl.loop(0, tiles)
        def _(i):
            part = jnp.zeros((TILE, 128), jnp.float32)
            for c in range(width // 128):
                v = xs[tile_rows(i), pl.ds(c * 128, 128)].astype(jnp.float32)
                part = part + v * v
            ss_own[layer, pl.ds(i, 1)] = jnp.sum(part.T, axis=0, keepdims=True)

    def ss_copy(layer, p):
        return pltpu.make_async_remote_copy(
            ss_own.at[layer], ss_in.at[layer, p - 1], ss_send.at[layer, p - 1], ss_recv.at[layer, p - 1],
            device_id=(sp, lax.rem(tp + p, n_tp)), device_id_type=MESH)

    def send_sums(layer):
        square_sums(layer)
        for p in range(1, n_tp):
            ss_copy(layer, p).start()

    def wait_sums(layer):
        for p in range(1, n_tp):
            ss_copy(layer, p).wait()

    def normalise(layer, lo, hi):
        @pl.loop(lo, hi)
        def _(i):
            total = ss_own[layer, pl.ds(i, 1)]
            for p in range(1, n_tp):
                total = total + ss_in[layer, p - 1, pl.ds(i, 1)]
            factor = lax.rsqrt(total / D + NORM_EPS)
            pos = base_pos + i * TILE + lax.broadcasted_iota(jnp.int32, (1, TILE), 1)
            factor = jnp.where((pos >= 0) & (pos < seq_total), factor, 0.0)
            column = jnp.broadcast_to(factor, (TILE, TILE)).T
            for c in range(width // 128):
                cols = pl.ds(c * 128, 128)
                v = xs[tile_rows(i), cols].astype(jnp.float32)
                g = gain_ref[layer : layer + 1, cols].astype(jnp.float32)
                ns[pl.ds(pl.multiple_of(PAD + i * TILE, 64), TILE), cols] = (v * column * g).astype(jnp.bfloat16)

    window = TILE + 2 * PAD

    def pool(lo, hi):
        @pl.loop(lo, hi)
        def _(i):
            offset = (
                lax.broadcasted_iota(jnp.int32, (TILE, window), 1)
                - lax.broadcasted_iota(jnp.int32, (TILE, window), 0)
                - PAD
            )
            pos = base_pos + i * TILE + lax.broadcasted_iota(jnp.int32, (TILE, window), 0)
            count = jnp.minimum(pos + half, seq_total) - jnp.maximum(pos - half, 0)
            count = jnp.maximum(count, 1).astype(jnp.float32)
            band = jnp.where((offset >= -half) & (offset < half), 1.0, 0.0)
            band = (band - jnp.where(offset == 0, count, 0.0)).astype(jnp.bfloat16)
            inverse = 1.0 / count[:, :1]
            rows_in = pl.ds(pl.multiple_of(i * TILE, TILE), window)
            for c in range(width // 256):
                cols = pl.ds(c * 256, 256)
                sums = jnp.dot(band, ns[rows_in, cols], preferred_element_type=jnp.float32)
                ps[tile_rows(i), cols] = (sums * inverse).astype(jnp.bfloat16)

    def mix(layer, first_row, block, first, columns):
        cols = pl.ds(first, columns)
        at = pl.ds(pl.multiple_of(first_row, 64), block)
        branch = jnp.dot(ps[at], ws[layer, :, cols], preferred_element_type=jnp.float32)
        s = scale_ref[layer : layer + 1, cols].astype(jnp.float32)
        mixed = (xs[at, cols].astype(jnp.float32) + branch * s).astype(jnp.bfloat16)
        xs[at, cols] = mixed

    third = tiles // 3
    thirds = [(0, third), (third, 2 * third), (2 * third, tiles)]

    def mix_block(layer, lo, hi):
        def run():
            for c in range(width // 256):
                mix(layer, lo * TILE, (hi - lo) * TILE, c * 256, 256)
        return run

    def prepare(layer):
        work = [lambda: send_sums(layer), lambda: None]
        first = [True]

        def norm(lo, hi):
            if first[0]:
                wait_sums(layer)
                first[0] = False
            normalise(layer, lo, hi)

        work += [functools.partial(norm, lo, hi) for lo, hi in thirds]
        work += [functools.partial(pool, lo, hi) for lo, hi in thirds]
        return work

    def start_work():
        x_load.wait()
        gain_load.wait()
        scale_load.wait()
        pl.when(has_prev)(lambda: to_next.wait_recv())
        pl.when(has_next)(lambda: to_prev.wait_recv())

    if in_kernel:
        w_loads[0].wait()
        loaded = [0]

        def own(u):
            if units[u][0] > loaded[0]:
                loaded[0] = units[u][0]
                w_loads[loaded[0]].wait()
            send_own(u)

        tasks = [start_work] + prepare(0)

        def next_layer(layer):
            while tasks:
                tasks.pop(0)()
            for v in range(len(units)):
                if units[v][0] == layer - 1:
                    arrive_across(v)
            tasks.extend([mix_block(layer - 1, lo, hi) for lo, hi in thirds] + prepare(layer))

        events = []
        place = 0
        for u in range(len(units)):
            events.append((place - LEAD, 0, u, functools.partial(own, u)))
            if units[u][3]:
                events.append((place - EARLY, 1, u, functools.partial(pass_own_row, u)))
            for step in range(1, line):
                events.append((place + SKEW * (step - 1), 2 + step, u, functools.partial(forward, u, step)))
            place += units[u][2] // (width // 8)
        for layer in range(1, layers):
            events.append((8 * layer + MIX_AT, 2, 0, functools.partial(next_layer, layer)))
        for _, kind, _, event in sorted(events, key=lambda e: e[:3]):
            event()
            if kind > 2 and tasks:
                tasks.pop(0)()
        while tasks:
            tasks.pop(0)()
    else:
        start_work()
        for layer in range(layers):
            for task in prepare(layer):
                task()
            w_loads[layer].wait()
            if layer < layers - 1:
                for lo, hi in thirds:
                    mix_block(layer, lo, hi)()

    outs = []
    for u, (layer, first, columns, _) in enumerate(units):
        if layer < layers - 1:
            continue
        if in_kernel:
            arrive_across(u)

        @pl.loop(0, rows // 256)
        def _(i):
            mix(layer, PAD + i * 256, 256, first, columns)

        outs.append(pltpu.make_async_copy(
            xs.at[pl.ds(PAD, rows), pl.ds(first, columns)], out_ref.at[:, pl.ds(first, columns)], out_sem.at[len(outs)]))
        outs[-1].start()

    pl.when(has_next)(lambda: to_next.wait_send())
    pl.when(has_prev)(lambda: to_prev.wait_send())
    if in_kernel:
        for u in range(len(units)):
            along = units[u][3]
            for j in range(line):
                def done(way, col):
                    copy(way, u, j, col).wait_send()

                @pl.when(has_down & (j >= z))
                def _():
                    done(DOWN, y)
                    if along:
                        done(DOWN, 1 - y)

                @pl.when(has_up & (j <= z))
                def _():
                    done(UP, y)
                    if along:
                        done(UP, 1 - y)

                if along:
                    pl.when(z == j)(lambda: done(ACROSS, y))
                else:
                    done(ACROSS, y)
    for out in outs:
        out.wait()


def solution(mesh):
    n_sp, n_tp = mesh.shape["sp"], mesh.shape["tp"]
    in_kernel = n_sp % 2 == 0 and n_sp <= 16

    def local(stream, norm_gain, pool_weight, pool_scale):
        rows, _ = stream.shape
        layers, per_dev, shard_rows, width = pool_weight.shape
        assert per_dev == 1 and n_tp == POOL_GROUPS
        if not in_kernel:
            pool_weight = lax.all_gather(pool_weight, "sp", axis=2, tiled=True)
        total_rows = rows + 2 * PAD
        units = len(unit_list(layers, width)) if in_kernel else 1
        dma = pltpu.SemaphoreType.DMA
        hbm = pl.BlockSpec(memory_space=pltpu.HBM)
        return pl.pallas_call(
            functools.partial(kernel, (layers, rows, width, shard_rows, n_sp, n_tp, in_kernel)),
            out_shape=jax.ShapeDtypeStruct((rows, width), jnp.bfloat16),
            in_specs=[hbm] * 4,
            out_specs=hbm,
            scratch_shapes=[
                pltpu.VMEM((layers, width), jnp.bfloat16),
                pltpu.VMEM((layers, width), jnp.bfloat16),
                pltpu.VMEM((total_rows, width), jnp.bfloat16),
                pltpu.VMEM((total_rows + 2 * PAD, width), jnp.bfloat16),
                pltpu.VMEM((total_rows, width), jnp.bfloat16),
                pltpu.VMEM((layers, width, width), jnp.bfloat16),
                pltpu.VMEM((layers, 16, TILE), jnp.float32),
                pltpu.VMEM((layers, n_tp - 1, 16, TILE), jnp.float32),
                dma((layers + 3,)),
                dma((2,)),
                dma((2,)),
                dma((layers, n_tp - 1)),
                dma((layers, n_tp - 1)),
                dma((3, units, n_sp)),
                dma((units, n_sp)),
                dma((4,)),
            ],
            compiler_params=pltpu.CompilerParams(
                collective_id=0, has_side_effects=True, vmem_limit_bytes=60 * 2**20
            ),
        )(stream, pool_weight, norm_gain, pool_scale)

    placed = (P("sp", "tp"), P(None, "tp"), P(None, "tp", "sp", None), P(None, "tp"))
    return jax.shard_map(
        local, mesh=mesh, in_specs=placed, out_specs=P("sp", "tp"), check_vma=False
    )
```
